32 devices in a mesh: grp: 2 (over y), sp: 4 (over z), tp: 4 (over x, core).
Axes of the slice: x: 2, y: 2, z: 4, core: 2. Of those that a mesh axis runs over, the one named last changes fastest.
Arguments:
- prompt: bfloat16 [8, 6144, 2048], P('grp', 'sp'), parts along dimension 0, may hold values from -6 to 6
- w_key: bfloat16 [2048, 2048], P('sp', 'tp'), may hold values from -0.125 to 0.125
- w_value: bfloat16 [2048, 2048], P('sp', 'tp'), may hold values from -0.125 to 0.125
- query_new: bfloat16 [8, 2048], P('grp', 'tp'), parts along dimension 0, may hold values from -150 to 150
- key_new: bfloat16 [8, 2048], P('grp', 'tp'), parts along dimension 0, may hold values from -15 to 15
- value_new: bfloat16 [8, 2048], P('grp', 'tp'), parts along dimension 0, may hold values from -6 to 6
- mix_lambda: float32 [16], P('tp'), may hold values from 0.3 to 0.8
- head_gain: float32 [128], replicated, may hold values from 0.1 to 1.9
Outputs:
- key_cache: bfloat16 [8, 4, 1536, 2048], P(('grp', 'sp'), None, None, 'tp'), parts along dimension 0
- value_cache: bfloat16 [8, 4, 1536, 2048], P(('grp', 'sp'), None, None, 'tp'), parts along dimension 0
- first_read: bfloat16 [8, 2048], P('grp', 'tp'), parts along dimension 0
The draws below stay inside these ranges and needn't reach their ends.
There are 2 independent parts, one for each index of `grp`. The reference program is written for one: setup_inputs(seed, part) draws one part's arguments, and reference() takes and returns one part's arrays. A program takes and returns all parts, laid end to end along the dimension named above; an argument that names none is the same for every part. Nothing has to cross between parts.
All inputs are finite; a program needn't handle non-finite values.
Results may differ from the reference program's by a relative error of at most 0.0065.
The reference program's roundings to bfloat16 on the way (of `keys`, `values` and `mixed`) count: a program that leaves them out, or rounds other values in their place, can miss the bound.
Values may be sent and summed in bfloat16 or wider, within the bound.
A program may use at most 128 MiB of HBM per device.

```python
import jax
import jax.numpy as jnp
from jax import lax

D = 2048
HEADS = 16
HALF = 64
VDIM = 128
SEQS = 4
LEN = 6144
N_SP = 4


def draw_query_new(key, part):
    base = jax.random.normal(key, (SEQS, HEADS, 2 * HALF), jnp.float32) * 1.75
    return jnp.clip(base, -10.0, 10.0).reshape(SEQS, HEADS * 2 * HALF).astype(jnp.bfloat16)


def levels(own_key, extent, pieces, least, high):
    def one(position, blocks):
        steps = jax.random.uniform(jax.random.fold_in(jax.random.fold_in(own_key, 6), position), (blocks,), jnp.float32, least / len(pieces), high / len(pieces))
        return jnp.repeat(jnp.exp(steps), extent[position] // blocks).reshape((-1,) + (1,) * (len(extent) - position - 1))

    gain = one(*pieces[0])
    for cut in pieces[1:]:
        gain = gain * one(*cut)
    return gain


def scatter_about(stream_key, shape, width, limit, cuts=(), kind=jnp.bfloat16):
    array = jax.random.normal(stream_key, shape, jnp.float32) * width
    if len(cuts) > 0:
        array = levels(stream_key, shape, cuts, -0.22, 0.18) * array
    return jnp.clip(array, min=-limit, max=limit).astype(kind)


def setup_inputs(seed: int = 0, part: int = 0) -> dict:
    seeds = jax.random.split(jax.random.key(seed), 9)
    own_keys = jax.random.split(jax.random.fold_in(seeds[8], part), 9)
    return {
        "prompt": scatter_about(own_keys[0], (SEQS, LEN, D), 1.0, 6.0, ((1, 4),)),
        "w_key": scatter_about(seeds[1], (D, HEADS * 2 * HALF), D ** -0.5, 0.125, ((0, 4), (1, 4))),
        "w_value": scatter_about(seeds[2], (D, HEADS * VDIM), D ** -0.5, 0.125, ((0, 4), (1, 4))),
        "query_new": draw_query_new(jax.random.fold_in(jax.random.fold_in(seeds[8], part), 71), part),
        "key_new": scatter_about(own_keys[4], (SEQS, HEADS * 2 * HALF), 2.5, 15.0, ((1, 4),)),
        "value_new": scatter_about(own_keys[5], (SEQS, HEADS * VDIM), 1.0, 6.0, ((1, 4),)),
        "mix_lambda": jnp.clip(0.3 + 0.5 * jax.random.uniform(seeds[6], (HEADS,), jnp.float32) ** levels(seeds[6], (HEADS,), ((0, 4),), -0.2, 0.2), 0.3, 0.8),
        "head_gain": jnp.clip(1.0 + 0.18 * jax.random.normal(seeds[7], (VDIM,), jnp.float32), 0.1, 1.9),
    }


def reference(prompt, w_key, w_value, query_new, key_new, value_new, mix_lambda, head_gain):
    rows = prompt.reshape(SEQS * LEN, D)
    keys = jnp.dot(rows, w_key, preferred_element_type=jnp.float32).astype(jnp.bfloat16)
    values = jnp.dot(rows, w_value, preferred_element_type=jnp.float32).astype(jnp.bfloat16)
    keys = keys.reshape(SEQS, LEN, HEADS * 2 * HALF)
    values = values.reshape(SEQS, LEN, HEADS * VDIM)
    scale = HALF ** (-0.5)

    def one_prompt(args):
        query, fresh_key, fresh_value, cached_keys, cached_values = args
        q_parts = query.astype(jnp.float32).reshape(HEADS, 2, HALF)
        k_parts = cached_keys.astype(jnp.float32).reshape(LEN, HEADS, 2, HALF)
        scores = jnp.einsum('hmc,lhmc->hml', q_parts, k_parts) * scale
        fresh = lax.optimization_barrier(jnp.sum(q_parts * fresh_key.astype(jnp.float32).reshape(HEADS, 2, HALF), axis=-1)) * scale
        top = jnp.maximum(lax.optimization_barrier(jnp.max(scores, axis=-1)), fresh)
        weights = jnp.exp(scores - top[..., None])
        own = jnp.exp(fresh - top)
        total = lax.optimization_barrier(jnp.sum(weights, axis=-1)) + own
        probs = weights / total[..., None]
        own_prob = own / total
        mixed = (probs[:, 0] - mix_lambda[:, None] * probs[:, 1]).astype(jnp.bfloat16)
        own_mixed = (own_prob[:, 0] - mix_lambda * own_prob[:, 1]).astype(jnp.bfloat16)
        value_parts = cached_values.astype(jnp.float32).reshape(LEN, HEADS, VDIM)
        reads = jnp.einsum('hl,lhv->hv', mixed.astype(jnp.float32), value_parts)
        reads = reads + own_mixed.astype(jnp.float32)[:, None] * fresh_value.astype(jnp.float32).reshape(HEADS, VDIM)
        mean = lax.optimization_barrier(jnp.mean(reads * reads, axis=-1, keepdims=True))
        normed = reads * lax.rsqrt(mean + 1e-06) * head_gain
        return normed.reshape(HEADS * VDIM).astype(jnp.bfloat16)
    first_read = lax.map(one_prompt, (query_new, key_new, value_new, keys, values))
    group = N_SP // SEQS
    sub = LEN // N_SP // group
    key_cache = keys.reshape(SEQS, N_SP, group, sub, HEADS * 2 * HALF).transpose(0, 2, 1, 3, 4)
    key_cache = key_cache.reshape(SEQS * group, N_SP, sub, HEADS * 2 * HALF)
    value_cache = values.reshape(SEQS, N_SP, group, sub, HEADS * VDIM).transpose(0, 2, 1, 3, 4)
    value_cache = value_cache.reshape(SEQS * group, N_SP, sub, HEADS * VDIM)
    return (key_cache, value_cache, first_read)
```

```python
import functools

import jax
import jax.numpy as jnp
from jax import lax
from jax.experimental import pallas as pl
from jax.experimental.pallas import tpu as pltpu
from jax.sharding import PartitionSpec as P

HALF = 64
VDIM = 128
MESH = pl.DeviceIdType.MESH
CHUNKS = 6
LAG_X = 1
LAG_C = 2


def combined_all(part, axis, combine):
    gathered = jax.tree.map(lambda a: lax.all_gather(a, axis), part)

    def take(source):
        return jax.tree.map(lambda a: lax.dynamic_index_in_dim(a, source, 0, False), gathered)

    return lax.fori_loop(
        1, lax.axis_size(axis), lambda source, state: combine(state, take(source)), take(0)
    )


def project(rows, w_key, w_value):
    keys = jnp.dot(
        rows, lax.all_gather(w_key, "sp", axis=0, tiled=True), preferred_element_type=jnp.float32
    )
    values = jnp.dot(
        rows, lax.all_gather(w_value, "sp", axis=0, tiled=True), preferred_element_type=jnp.float32
    )
    return (keys.astype(jnp.bfloat16), values.astype(jnp.bfloat16))


def score_maps(query, keys):
    count, span = (keys.shape[0], keys.shape[1])
    heads = query.shape[1] // (2 * HALF)
    q_parts = query.reshape(count, heads, 2, HALF)
    k_parts = keys.reshape(count, span, heads, 2, HALF)
    return jnp.einsum(
        "shmc,slhmc->shml", q_parts, k_parts, preferred_element_type=jnp.float32
    ) * HALF ** (-0.5)


def own_scores(query, fresh_key):
    count = query.shape[0]
    heads = query.shape[1] // (2 * HALF)
    q_parts = query.astype(jnp.float32).reshape(count, heads, 2, HALF)
    k_parts = fresh_key.astype(jnp.float32).reshape(count, heads, 2, HALF)
    return jnp.sum(q_parts * k_parts, axis=-1) * HALF ** (-0.5)


def finish(reads, head_gain):
    mean = jnp.mean(reads * reads, axis=-1, keepdims=True)
    normed = reads * lax.rsqrt(mean + 1e-06) * head_gain
    return normed.reshape(reads.shape[0], -1).astype(jnp.bfloat16)


def join_totals(first, second):
    top = jnp.maximum(first[0], second[0])
    return (top, first[1] * jnp.exp(first[0] - top) + second[1] * jnp.exp(second[0] - top))


def placed(part_rows, prompts, first, fill):
    base = jnp.full((prompts,) + part_rows.shape[1:], fill, jnp.float32)
    return lax.dynamic_update_slice_in_dim(base, part_rows, first, 0)


def cache_read(query_new, key_new, value_new, keys, values, mix_lambda, head_gain, first):
    count, span = (keys.shape[0], keys.shape[1])
    prompts = query_new.shape[0]
    heads = mix_lambda.shape[0]
    query = lax.dynamic_slice_in_dim(query_new, first, count, 0)
    scores = score_maps(query, keys)
    fresh_all = own_scores(query_new, key_new)
    fresh = lax.dynamic_slice_in_dim(fresh_all, first, count, 0)
    local_top = jnp.maximum(jnp.max(scores, axis=-1), fresh)
    local_total = jnp.sum(jnp.exp(scores - local_top[..., None]), axis=-1)
    top_all, cache_total = combined_all(
        (placed(local_top, prompts, first, -1e30), placed(local_total, prompts, first, 0.0)),
        "sp",
        join_totals,
    )
    own = jnp.exp(fresh_all - top_all)
    total_all = cache_total + own
    top = lax.dynamic_slice_in_dim(top_all, first, count, 0)
    total = lax.dynamic_slice_in_dim(total_all, first, count, 0)
    probs = jnp.exp(scores - top[..., None]) / total[..., None]
    mixed = (probs[:, :, 0] - mix_lambda[None, :, None] * probs[:, :, 1]).astype(jnp.bfloat16)
    value_parts = values.reshape(count, span, heads, VDIM)
    partial_value = jnp.einsum(
        "shl,slhv->shv", mixed, value_parts, preferred_element_type=jnp.float32
    )
    reads = lax.psum(placed(partial_value, prompts, first, 0.0), "sp")
    own_prob = own / total_all
    own_mixed = (own_prob[:, :, 0] - mix_lambda[None, :] * own_prob[:, :, 1]).astype(jnp.bfloat16)
    reads = reads + own_mixed.astype(jnp.float32)[..., None] * value_new.astype(
        jnp.float32
    ).reshape(prompts, heads, VDIM)
    return finish(reads, head_gain)


def block_read(
    query_new, key_new, value_new, key_cache, value_cache, mix_lambda, head_gain, spread
):
    blocks, sub = (key_cache.shape[1], key_cache.shape[2])
    first = lax.axis_index("sp") // spread
    keys = key_cache.reshape(1, blocks * sub, -1)
    values = value_cache.reshape(1, blocks * sub, -1)
    return cache_read(query_new, key_new, value_new, keys, values, mix_lambda, head_gain, first)


def body(prompt, w_key, w_value, query_new, key_new, value_new, mix_lambda, head_gain):
    count, piece, width = prompt.shape
    spread = lax.axis_size("sp") // count
    sub = piece // spread
    keys, values = project(prompt.reshape(count * piece, width), w_key, w_value)
    key_blocks = keys.reshape(count * spread, 1, sub, -1)
    value_blocks = values.reshape(count * spread, 1, sub, -1)
    key_cache, value_cache = (
        lax.all_to_all(key_blocks, "sp", split_axis=0, concat_axis=1, tiled=True),
        lax.all_to_all(value_blocks, "sp", split_axis=0, concat_axis=1, tiled=True),
    )
    first_read = block_read(
        query_new, key_new, value_new, key_cache, value_cache, mix_lambda, head_gain, spread
    )
    return (key_cache, value_cache, first_read)


def gather_kernel(
    sizes, prompt, w_key, w_value, keys, values,
    rows_in, weights, k_buf, v_buf,
    z_send, z_recv, x_send, x_recv, d_send, d_recv, e_send, e_recv,
    wr_send, wr_recv, wl_send, wl_recv, wy_send, wy_recv, local, out_sem,
):
    n, chunks, tile, quarter = sizes
    me = lax.axis_index("sp")
    tp = lax.axis_index("tp")
    grp = lax.axis_index("grp")
    across = lax.rem(tp + 2, 4)
    sibling = tp + 1 - 2 * lax.rem(tp, 2)
    far = lax.rem(sibling + 2, 4)
    depth, cols = w_key.shape
    half = depth // 2
    mats = (w_key, w_value)

    def rows(j, q):
        return pl.ds(pl.multiple_of(j * tile + q * quarter, quarter), quarter)

    barrier = pltpu.get_barrier_semaphore()
    for step in range(1, n):
        pl.semaphore_signal(
            barrier, inc=1, device_id={"sp": lax.rem(me + step, n)}, device_id_type=MESH
        )
    pl.semaphore_signal(barrier, inc=1, device_id={"tp": across}, device_id_type=MESH)
    pl.semaphore_signal(barrier, inc=1, device_id={"tp": sibling}, device_id_type=MESH)
    pl.semaphore_signal(barrier, inc=1, device_id={"grp": 1 - grp}, device_id_type=MESH)
    pl.semaphore_wait(barrier, n + 2)

    def w_slot(src, m, g):
        return weights.at[pl.ds(pl.multiple_of(src * depth + g * half, half), half),
                          pl.ds(m * cols, cols)]

    def w_hop(src, m, to, send, recv, own):
        origin = mats[m].at[pl.ds(pl.multiple_of(grp * half, half), half)] if own else w_slot(src, m, grp)
        return pltpu.make_async_remote_copy(
            src_ref=origin, dst_ref=w_slot(src, m, grp),
            send_sem=send.at[src * 2 + m], recv_sem=recv.at[src * 2 + m],
            device_id={"sp": to}, device_id_type=MESH,
        )

    def w_side(src, m, g):
        return pltpu.make_async_remote_copy(
            src_ref=w_slot(src, m, g), dst_ref=w_slot(src, m, g),
            send_sem=wy_send.at[src * 2 + m], recv_sem=wy_recv.at[src * 2 + m],
            device_id={"grp": 1 - grp}, device_id_type=MESH,
        )

    def z_copy(src, dst, j):
        return pltpu.make_async_remote_copy(
            src_ref=prompt.at[dst, rows(j, tp)], dst_ref=rows_in.at[src, rows(j, tp)],
            send_sem=z_send.at[dst * chunks + j], recv_sem=z_recv.at[src * chunks + j],
            device_id={"sp": dst}, device_id_type=MESH,
        )

    def side_copy(src, j, q, to, send, recv):
        return pltpu.make_async_remote_copy(
            src_ref=rows_in.at[src, rows(j, q)], dst_ref=rows_in.at[src, rows(j, q)],
            send_sem=send.at[src * chunks + j], recv_sem=recv.at[src * chunks + j],
            device_id={"tp": to}, device_id_type=MESH,
        )

    def right_sends():
        def send(i, carry):
            z_copy(me, me + 1 + i // chunks, lax.rem(i, chunks)).start()
            return carry
        lax.fori_loop(0, (n - 1 - me) * chunks, send, 0)

    def left_sends():
        def send(i, carry):
            z_copy(me, me - 1 - i // chunks, lax.rem(i, chunks)).start()
            return carry
        lax.fori_loop(0, me * chunks, send, 0)

    for m in range(2):
        @pl.when(me + 1 < n)
        def _():
            w_hop(me, m, me + 1, wr_send, wr_recv, True).start()

        @pl.when(me > 0)
        def _():
            w_hop(me, m, me - 1, wl_send, wl_recv, True).start()

    own_w = [
        pltpu.make_async_copy(
            mats[m],
            weights.at[pl.ds(pl.multiple_of(me * depth, depth), depth), pl.ds(m * cols, cols)],
            local.at[m],
        )
        for m in range(2)
    ]
    own_rows = pltpu.make_async_copy(prompt.at[me], rows_in.at[me], local.at[2])
    for copy in own_w:
        copy.start()
    own_rows.start()

    @pl.when(me == 0)
    def _():
        right_sends()

    @pl.when(me == n - 1)
    def _():
        left_sends()

    for d in range(1, n):
        @pl.when(me - d >= 0)
        def _():
            for m in range(2):
                w_hop(me - d, m, me, wr_send, wr_recv, False).wait_recv()

                @pl.when(me + 1 < n)
                def _():
                    w_hop(me - d, m, me + 1, wr_send, wr_recv, False).start()

                w_side(me - d, m, grp).start()

        @pl.when(me + d < n)
        def _():
            for m in range(2):
                w_hop(me + d, m, me, wl_send, wl_recv, False).wait_recv()

                @pl.when(me > 0)
                def _():
                    w_hop(me + d, m, me - 1, wl_send, wl_recv, False).start()

                w_side(me + d, m, grp).start()

        @pl.when(me == d)
        def _():
            right_sends()

        @pl.when(n - 1 - me == d)
        def _():
            left_sends()

    for step in range(1, n):
        src = lax.rem(me + step, n)
        for m in range(2):
            w_side(src, m, 1 - grp).wait_recv()
    for copy in own_w:
        copy.wait()
    own_rows.wait()

    def out_copies(slot, src, j):
        where = pl.ds(pl.multiple_of(j * tile, tile), tile)
        return (
            pltpu.make_async_copy(k_buf.at[slot], keys.at[src, where], out_sem.at[slot]),
            pltpu.make_async_copy(v_buf.at[slot], values.at[src, where], out_sem.at[slot + 2]),
        )

    def compute(slot, busy, src, j):
        block = rows_in[src, pl.ds(pl.multiple_of(j * tile, tile), tile), :]
        both = jnp.dot(block, weights[...], preferred_element_type=jnp.float32)

        @pl.when(busy)
        def _():
            for copy in out_copies(slot, src, j):
                copy.wait()

        k_buf[slot] = both[:, :cols].astype(jnp.bfloat16)
        v_buf[slot] = both[:, cols:].astype(jnp.bfloat16)
        for copy in out_copies(slot, src, j):
            copy.start()

    inner = jnp.minimum(me, n - 1 - me)

    def order(k):
        pairs = 2 * inner * chunks
        r = lax.rem(k, 2 * chunks)
        two = me + (k // (2 * chunks) + 1) * (1 - 2 * lax.rem(r, 2))
        s = k - pairs
        d = inner + 1 + s // chunks
        one = jnp.where(me > n - 1 - me, me - d, me + d)
        both = k < pairs
        return jnp.where(both, two, one), jnp.where(both, r // 2, lax.rem(s, chunks))

    total = (n - 1) * chunks

    def step(k, carry):
        @pl.when(k < total)
        def _():
            src, j = order(k)
            z_copy(src, me, j).wait_recv()
            side_copy(src, j, tp, across, x_send, x_recv).start()
            side_copy(src, j, tp, sibling, d_send, d_recv).start()

        @pl.when((k >= LAG_X) & (k < total + LAG_X))
        def _():
            src, j = order(k - LAG_X)
            side_copy(src, j, across, across, x_send, x_recv).wait_recv()
            side_copy(src, j, across, sibling, e_send, e_recv).start()

        @pl.when(k < chunks)
        def _():
            compute(0, k > 0, me, k)

        @pl.when(k >= LAG_C)
        def _():
            src, j = order(k - LAG_C)
            side_copy(src, j, sibling, sibling, d_send, d_recv).wait_recv()
            side_copy(src, j, far, sibling, e_send, e_recv).wait_recv()
            compute(1, k > LAG_C, src, j)

        return carry

    lax.fori_loop(0, total + LAG_C, step, 0)

    for slot in range(2):
        for copy in out_copies(slot, me, 0):
            copy.wait()

    def drain(k, carry):
        src, j = order(k)
        z_copy(me, src, j).wait_send()
        side_copy(src, j, tp, across, x_send, x_recv).wait_send()
        side_copy(src, j, tp, sibling, d_send, d_recv).wait_send()
        side_copy(src, j, across, sibling, e_send, e_recv).wait_send()
        return carry

    lax.fori_loop(0, total, drain, 0)
    for step_ in range(1, n):
        src = lax.rem(me + step_, n)
        for m in range(2):
            w_side(src, m, grp).wait_send()
    for d in range(n):
        for m in range(2):
            @pl.when((me - d >= 0) & (me + 1 < n))
            def _():
                w_hop(me - d, m, me + 1, wr_send, wr_recv, False).wait_send()

            @pl.when((me + d < n) & (me > 0))
            def _():
                w_hop(me + d, m, me - 1, wl_send, wl_recv, False).wait_send()


def gather_project(n, prompt, w_key, w_value):
    count, piece, width = prompt.shape
    depth, cols = w_key.shape
    tile = piece // CHUNKS
    quarter = tile // 4
    dma = pltpu.SemaphoreType.DMA
    steps = n * CHUNKS
    out = jax.ShapeDtypeStruct((n, piece, cols), jnp.bfloat16)
    hbm = pl.BlockSpec(memory_space=pl.ANY)
    return pl.pallas_call(
        functools.partial(gather_kernel, (n, CHUNKS, tile, quarter)),
        out_shape=(out, out),
        in_specs=[hbm] * 3,
        out_specs=(hbm, hbm),
        scratch_shapes=[
            pltpu.VMEM((n, piece, width), jnp.bfloat16),
            pltpu.VMEM((n * depth, 2 * cols), jnp.bfloat16),
            pltpu.VMEM((2, tile, cols), jnp.bfloat16),
            pltpu.VMEM((2, tile, cols), jnp.bfloat16),
        ]
        + [dma((steps,))] * 8
        + [dma((2 * n,))] * 6
        + [dma((3,)), dma((4,))],
        compiler_params=pltpu.CompilerParams(
            collective_id=0, has_side_effects=True, vmem_limit_bytes=56 * 2**20
        ),
    )(prompt, w_key, w_value)


def read_kernel(
    pieces, query, key_new, value_new, lam, gain, keys_in, values_in, keys, values, read,
    k_all, v_all, scores, in_sem, out_sem,
):
    span, cols = k_all.shape
    tile = span // pieces
    heads = cols // VDIM
    me = lax.axis_index("sp")

    def load(i):
        where = pl.ds(i * tile, tile)
        return (
            pltpu.make_async_copy(keys_in.at[where], k_all.at[where], in_sem.at[2 * i]),
            pltpu.make_async_copy(values_in.at[where], v_all.at[where], in_sem.at[2 * i + 1]),
        )

    def store(i):
        where = pl.ds(i * tile, tile)
        return (
            pltpu.make_async_copy(k_all.at[where], keys.at[where], out_sem.at[2 * i]),
            pltpu.make_async_copy(v_all.at[where], values.at[where], out_sem.at[2 * i + 1]),
        )

    for i in range(pieces):
        for copy in load(i):
            copy.start()

    def mine(ref):
        whole = ref[...].astype(jnp.float32)
        here = lax.broadcasted_iota(jnp.int32, whole.shape, 0) == me
        return jnp.sum(jnp.where(here, whole, 0.0), axis=0, keepdims=True)

    shape = (2 * heads, cols)
    row = lax.broadcasted_iota(jnp.int32, shape, 0)
    group = lax.broadcasted_iota(jnp.int32, shape, 1) // HALF
    part = jnp.where(row < heads, 2 * row, 2 * (row - heads) + 1) == group
    q_row = mine(query)
    q_mat = jnp.where(part, jnp.broadcast_to(q_row, shape), 0.0)
    scale = HALF ** (-0.5)
    fresh = jnp.sum(q_mat * mine(key_new), axis=1, keepdims=True) * scale
    q_low = q_mat.astype(jnp.bfloat16)
    for i in range(pieces):
        for copy in load(i):
            copy.wait()
        for copy in store(i):
            copy.start()
        scores[:, i * tile:(i + 1) * tile] = lax.dot_general(
            q_low, k_all[i * tile:(i + 1) * tile, :], (((1,), (1,)), ((), ())),
            preferred_element_type=jnp.float32,
        ) * scale
    s = scores[...]
    top = jnp.maximum(jnp.max(s, axis=1, keepdims=True), fresh)
    e = jnp.exp(s - top)
    own = jnp.exp(fresh - top)
    total = jnp.sum(e, axis=1, keepdims=True) + own
    w = e / total
    own = own / total
    mix = lam[...]
    mixed = (w[:heads] - mix * w[heads:]).astype(jnp.bfloat16)
    own_mixed = (own[:heads] - mix * own[heads:]).astype(jnp.bfloat16).astype(jnp.float32)
    o = jnp.dot(mixed, v_all[...], preferred_element_type=jnp.float32)
    o = o + own_mixed * mine(value_new)
    for h in range(heads):
        lanes = slice(h * VDIM, (h + 1) * VDIM)
        one = o[h:h + 1, lanes]
        mean = jnp.mean(one * one, axis=1, keepdims=True)
        read[:, lanes] = (one * lax.rsqrt(mean + 1e-06) * gain[...]).astype(jnp.bfloat16)
    for i in range(pieces):
        for copy in store(i):
            copy.wait()


def read_call(query, key_new, value_new, mix_lambda, head_gain, keys, values):
    span, cols = keys.shape
    heads = mix_lambda.shape[0]
    pieces = 12
    hbm = pl.BlockSpec(memory_space=pl.ANY)
    vmem = pl.BlockSpec(memory_space=pltpu.VMEM)
    out = jax.ShapeDtypeStruct((span, cols), jnp.bfloat16)
    dma = pltpu.SemaphoreType.DMA
    return pl.pallas_call(
        functools.partial(read_kernel, pieces),
        out_shape=(out, out, jax.ShapeDtypeStruct((1, cols), jnp.bfloat16)),
        in_specs=[vmem] * 5 + [hbm] * 2,
        out_specs=(hbm, hbm, vmem),
        scratch_shapes=[
            pltpu.VMEM((span, cols), jnp.bfloat16),
            pltpu.VMEM((span, cols), jnp.bfloat16),
            pltpu.VMEM((2 * heads, span), jnp.float32),
            dma((2 * pieces,)),
            dma((2 * pieces,)),
        ],
        compiler_params=pltpu.CompilerParams(vmem_limit_bytes=40 * 2**20),
    )(query, key_new, value_new, mix_lambda[:, None], head_gain[None, :], keys, values)


def fast_body(prompt, w_key, w_value, query_new, key_new, value_new, mix_lambda, head_gain):
    count, piece, width = prompt.shape
    n = lax.axis_size("sp")
    keys, values = gather_project(n, prompt, w_key, w_value)
    cols = keys.shape[-1]
    keys, values, read = read_call(
        query_new, key_new, value_new, mix_lambda, head_gain,
        keys.reshape(n * piece, cols), values.reshape(n * piece, cols),
    )
    return (
        keys.reshape(1, n, piece, cols),
        values.reshape(1, n, piece, cols),
        lax.all_gather(read, "sp", axis=0, tiled=True),
    )


def choose(mesh):
    def run(prompt, *rest):
        sizes = dict(mesh.shape)
        count, piece, width = prompt.shape
        rows = rest[0].shape[0]
        fits = (
            sizes["grp"] == 2
            and sizes["tp"] == 4
            and sizes["sp"] == count
            and count > 1
            and piece % (64 * CHUNKS) == 0
            and rows % 32 == 0
            and (count * piece) % 1536 == 0
            and count * piece * width * 2 <= 2**25
        )
        return (fast_body if fits else body)(prompt, *rest)

    return run


def solution(mesh):
    placed = (
        P("grp", "sp", None),
        P("sp", "tp"),
        P("sp", "tp"),
        P("grp", "tp"),
        P("grp", "tp"),
        P("grp", "tp"),
        P("tp"),
        P(),
    )
    return jax.shard_map(
        choose(mesh),
        mesh=mesh,
        in_specs=placed,
        out_specs=(
            P(("grp", "sp"), None, None, "tp"),
            P(("grp", "sp"), None, None, "tp"),
            P("grp", "tp"),
        ),
        check_vma=False,
    )
```

```python
import functools

import jax
import jax.numpy as jnp
from jax import lax
from jax.experimental import pallas as pl
from jax.experimental.pallas import tpu as pltpu
from jax.sharding import PartitionSpec as P

HALF = 64
VDIM = 128
MESH = pl.DeviceIdType.MESH
CHUNKS = 8
LAG_X = 1
LAG_C = 2
EARLY = 2
AHEAD = 24


def combined_all(part, axis, combine):
    gathered = jax.tree.map(lambda a: lax.all_gather(a, axis), part)

    def take(source):
        return jax.tree.map(lambda a: lax.dynamic_index_in_dim(a, source, 0, False), gathered)

    return lax.fori_loop(
        1, lax.axis_size(axis), lambda source, state: combine(state, take(source)), take(0)
    )


def project(rows, w_key, w_value):
    keys = jnp.dot(
        rows, lax.all_gather(w_key, "sp", axis=0, tiled=True), preferred_element_type=jnp.float32
    )
    values = jnp.dot(
        rows, lax.all_gather(w_value, "sp", axis=0, tiled=True), preferred_element_type=jnp.float32
    )
    return (keys.astype(jnp.bfloat16), values.astype(jnp.bfloat16))


def score_maps(query, keys):
    count, span = (keys.shape[0], keys.shape[1])
    heads = query.shape[1] // (2 * HALF)
    q_parts = query.reshape(count, heads, 2, HALF)
    k_parts = keys.reshape(count, span, heads, 2, HALF)
    return jnp.einsum(
        "shmc,slhmc->shml", q_parts, k_parts, preferred_element_type=jnp.float32
    ) * HALF ** (-0.5)


def own_scores(query, fresh_key):
    count = query.shape[0]
    heads = query.shape[1] // (2 * HALF)
    q_parts = query.astype(jnp.float32).reshape(count, heads, 2, HALF)
    k_parts = fresh_key.astype(jnp.float32).reshape(count, heads, 2, HALF)
    return jnp.sum(q_parts * k_parts, axis=-1) * HALF ** (-0.5)


def finish(reads, head_gain):
    mean = jnp.mean(reads * reads, axis=-1, keepdims=True)
    normed = reads * lax.rsqrt(mean + 1e-06) * head_gain
    return normed.reshape(reads.shape[0], -1).astype(jnp.bfloat16)


def join_totals(first, second):
    top = jnp.maximum(first[0], second[0])
    return (top, first[1] * jnp.exp(first[0] - top) + second[1] * jnp.exp(second[0] - top))


def placed(part_rows, prompts, first, fill):
    base = jnp.full((prompts,) + part_rows.shape[1:], fill, jnp.float32)
    return lax.dynamic_update_slice_in_dim(base, part_rows, first, 0)


def cache_read(query_new, key_new, value_new, keys, values, mix_lambda, head_gain, first):
    count, span = (keys.shape[0], keys.shape[1])
    prompts = query_new.shape[0]
    heads = mix_lambda.shape[0]
    query = lax.dynamic_slice_in_dim(query_new, first, count, 0)
    scores = score_maps(query, keys)
    fresh_all = own_scores(query_new, key_new)
    fresh = lax.dynamic_slice_in_dim(fresh_all, first, count, 0)
    local_top = jnp.maximum(jnp.max(scores, axis=-1), fresh)
    local_total = jnp.sum(jnp.exp(scores - local_top[..., None]), axis=-1)
    top_all, cache_total = combined_all(
        (placed(local_top, prompts, first, -1e30), placed(local_total, prompts, first, 0.0)),
        "sp",
        join_totals,
    )
    own = jnp.exp(fresh_all - top_all)
    total_all = cache_total + own
    top = lax.dynamic_slice_in_dim(top_all, first, count, 0)
    total = lax.dynamic_slice_in_dim(total_all, first, count, 0)
    probs = jnp.exp(scores - top[..., None]) / total[..., None]
    mixed = (probs[:, :, 0] - mix_lambda[None, :, None] * probs[:, :, 1]).astype(jnp.bfloat16)
    value_parts = values.reshape(count, span, heads, VDIM)
    partial_value = jnp.einsum(
        "shl,slhv->shv", mixed, value_parts, preferred_element_type=jnp.float32
    )
    reads = lax.psum(placed(partial_value, prompts, first, 0.0), "sp")
    own_prob = own / total_all
    own_mixed = (own_prob[:, :, 0] - mix_lambda[None, :] * own_prob[:, :, 1]).astype(jnp.bfloat16)
    reads = reads + own_mixed.astype(jnp.float32)[..., None] * value_new.astype(
        jnp.float32
    ).reshape(prompts, heads, VDIM)
    return finish(reads, head_gain)


def block_read(
    query_new, key_new, value_new, key_cache, value_cache, mix_lambda, head_gain, spread
):
    blocks, sub = (key_cache.shape[1], key_cache.shape[2])
    first = lax.axis_index("sp") // spread
    keys = key_cache.reshape(1, blocks * sub, -1)
    values = value_cache.reshape(1, blocks * sub, -1)
    return cache_read(query_new, key_new, value_new, keys, values, mix_lambda, head_gain, first)


def body(prompt, w_key, w_value, query_new, key_new, value_new, mix_lambda, head_gain):
    count, piece, width = prompt.shape
    spread = lax.axis_size("sp") // count
    sub = piece // spread
    keys, values = project(prompt.reshape(count * piece, width), w_key, w_value)
    key_blocks = keys.reshape(count * spread, 1, sub, -1)
    value_blocks = values.reshape(count * spread, 1, sub, -1)
    key_cache, value_cache = (
        lax.all_to_all(key_blocks, "sp", split_axis=0, concat_axis=1, tiled=True),
        lax.all_to_all(value_blocks, "sp", split_axis=0, concat_axis=1, tiled=True),
    )
    first_read = block_read(
        query_new, key_new, value_new, key_cache, value_cache, mix_lambda, head_gain, spread
    )
    return (key_cache, value_cache, first_read)


def gather_kernel(
    sizes, prompt, w_key, w_value, keys, values,
    rows_in, weights,
    z_send, z_recv, x_send, x_recv, d_send, d_recv, e_send, e_recv,
    wr_send, wr_recv, wl_send, wl_recv, wy_send, wy_recv, local,
):
    n, chunks, tile, quarter = sizes
    me = lax.axis_index("sp")
    tp = lax.axis_index("tp")
    grp = lax.axis_index("grp")
    across = lax.rem(tp + 2, 4)
    sibling = tp + 1 - 2 * lax.rem(tp, 2)
    far = lax.rem(sibling + 2, 4)
    depth, cols = w_key.shape
    half = depth // 2
    mats = (w_key, w_value)

    def rows(j, q):
        return pl.ds(pl.multiple_of(j * tile + q * quarter, quarter), quarter)

    barrier = pltpu.get_barrier_semaphore()
    for step in range(1, n):
        pl.semaphore_signal(
            barrier, inc=1, device_id={"sp": lax.rem(me + step, n)}, device_id_type=MESH
        )
    pl.semaphore_signal(barrier, inc=1, device_id={"tp": across}, device_id_type=MESH)
    pl.semaphore_signal(barrier, inc=1, device_id={"tp": sibling}, device_id_type=MESH)
    pl.semaphore_signal(barrier, inc=1, device_id={"grp": 1 - grp}, device_id_type=MESH)
    pl.semaphore_wait(barrier, n + 2)

    def w_slot(src, m, g):
        return weights.at[pl.ds(pl.multiple_of(src * depth + g * half, half), half),
                          pl.ds(m * cols, cols)]

    def w_hop(src, m, to, send, recv, own):
        origin = mats[m].at[pl.ds(pl.multiple_of(grp * half, half), half)] if own else w_slot(src, m, grp)
        return pltpu.make_async_remote_copy(
            src_ref=origin, dst_ref=w_slot(src, m, grp),
            send_sem=send.at[src * 2 + m], recv_sem=recv.at[src * 2 + m],
            device_id={"sp": to}, device_id_type=MESH,
        )

    def w_side(src, m, g):
        return pltpu.make_async_remote_copy(
            src_ref=w_slot(src, m, g), dst_ref=w_slot(src, m, g),
            send_sem=wy_send.at[src * 2 + m], recv_sem=wy_recv.at[src * 2 + m],
            device_id={"grp": 1 - grp}, device_id_type=MESH,
        )

    def z_copy(src, dst, j):
        return pltpu.make_async_remote_copy(
            src_ref=prompt.at[dst, rows(j, tp)], dst_ref=rows_in.at[src, rows(j, tp)],
            send_sem=z_send.at[dst * chunks + j], recv_sem=z_recv.at[src * chunks + j],
            device_id={"sp": dst}, device_id_type=MESH,
        )

    def side_copy(src, j, q, to, send, recv):
        return pltpu.make_async_remote_copy(
            src_ref=rows_in.at[src, rows(j, q)], dst_ref=rows_in.at[src, rows(j, q)],
            send_sem=send.at[src * chunks + j], recv_sem=recv.at[src * chunks + j],
            device_id={"tp": to}, device_id_type=MESH,
        )

    def right_send(i):
        @pl.when(i < (n - 1 - me) * chunks)
        def _():
            c = jnp.maximum(n - 1 - me, 1)
            z_copy(me, me + c - lax.rem(i, c), i // c).start()

    def left_send(i):
        @pl.when(i < me * chunks)
        def _():
            c = jnp.maximum(me, 1)
            z_copy(me, me - c + lax.rem(i, c), i // c).start()

    def both_sends(i, carry):
        right_send(i)
        left_send(i)
        return carry

    for m in range(2):
        @pl.when(me + 1 < n)
        def _():
            w_hop(me, m, me + 1, wr_send, wr_recv, True).start()

        @pl.when(me > 0)
        def _():
            w_hop(me, m, me - 1, wl_send, wl_recv, True).start()

    own_w = [
        pltpu.make_async_copy(
            mats[m],
            weights.at[pl.ds(pl.multiple_of(me * depth, depth), depth), pl.ds(m * cols, cols)],
            local.at[m],
        )
        for m in range(2)
    ]
    own_rows = pltpu.make_async_copy(prompt.at[me], rows_in.at[me], local.at[2])
    for copy in own_w:
        copy.start()
    own_rows.start()

    @pl.when(me == 0)
    def _():
        for i in range(EARLY):
            right_send(i)

    @pl.when(me == n - 1)
    def _():
        for i in range(EARLY):
            left_send(i)

    for d in range(1, n):
        @pl.when(me - d >= 0)
        def _():
            for m in range(2):
                w_hop(me - d, m, me, wr_send, wr_recv, False).wait_recv()

                @pl.when(me + 1 < n)
                def _():
                    w_hop(me - d, m, me + 1, wr_send, wr_recv, False).start()

                w_side(me - d, m, grp).start()

        @pl.when(me + d < n)
        def _():
            for m in range(2):
                w_hop(me + d, m, me, wl_send, wl_recv, False).wait_recv()

                @pl.when(me > 0)
                def _():
                    w_hop(me + d, m, me - 1, wl_send, wl_recv, False).start()

                w_side(me + d, m, grp).start()

        @pl.when(me == d)
        def _():
            for i in range(EARLY):
                right_send(i)

        @pl.when(n - 1 - me == d)
        def _():
            for i in range(EARLY):
                left_send(i)

    lax.fori_loop(EARLY, AHEAD, both_sends, 0)

    for step in range(1, n):
        src = lax.rem(me + step, n)
        for m in range(2):
            w_side(src, m, 1 - grp).wait_recv()
    for copy in own_w:
        copy.wait()
    own_rows.wait()

    def compute(src, j):
        where = pl.ds(pl.multiple_of(j * tile, tile), tile)
        both = jnp.dot(
            rows_in[src, where, :], weights[...], preferred_element_type=jnp.float32
        ).astype(jnp.bfloat16)
        keys[src, where, :] = both[:, :cols]
        values[src, where, :] = both[:, cols:]

    def order(k):
        return lax.rem(me + 1 + lax.rem(k, n - 1), n), k // (n - 1)

    total = (n - 1) * chunks

    def step(k, carry):
        both_sends(AHEAD + k, 0)

        @pl.when(k < total)
        def _():
            src, j = order(k)
            z_copy(src, me, j).wait_recv()
            side_copy(src, j, tp, across, x_send, x_recv).start()
            side_copy(src, j, tp, sibling, d_send, d_recv).start()

        @pl.when((k >= LAG_X) & (k < total + LAG_X))
        def _():
            src, j = order(k - LAG_X)
            side_copy(src, j, across, across, x_send, x_recv).wait_recv()
            side_copy(src, j, across, sibling, e_send, e_recv).start()

        @pl.when(k < chunks)
        def _():
            compute(me, k)

        @pl.when(k >= LAG_C)
        def _():
            src, j = order(k - LAG_C)
            side_copy(src, j, sibling, sibling, d_send, d_recv).wait_recv()
            side_copy(src, j, far, sibling, e_send, e_recv).wait_recv()
            compute(src, j)

        return carry

    lax.fori_loop(0, total + LAG_C, step, 0)

    def drain(k, carry):
        src, j = order(k)
        z_copy(me, src, j).wait_send()
        side_copy(src, j, tp, across, x_send, x_recv).wait_send()
        side_copy(src, j, tp, sibling, d_send, d_recv).wait_send()
        side_copy(src, j, across, sibling, e_send, e_recv).wait_send()
        return carry

    lax.fori_loop(0, total, drain, 0)
    for step_ in range(1, n):
        src = lax.rem(me + step_, n)
        for m in range(2):
            w_side(src, m, grp).wait_send()
    for d in range(n):
        for m in range(2):
            @pl.when((me - d >= 0) & (me + 1 < n))
            def _():
                w_hop(me - d, m, me + 1, wr_send, wr_recv, False).wait_send()

            @pl.when((me + d < n) & (me > 0))
            def _():
                w_hop(me + d, m, me - 1, wl_send, wl_recv, False).wait_send()


def gather_project(n, prompt, w_key, w_value):
    count, piece, width = prompt.shape
    depth, cols = w_key.shape
    tile = piece // CHUNKS
    quarter = tile // 4
    dma = pltpu.SemaphoreType.DMA
    steps = n * CHUNKS
    out = pltpu.VMEM((n, piece, cols), jnp.bfloat16)
    vmem = pl.BlockSpec(memory_space=pltpu.VMEM)
    hbm = pl.BlockSpec(memory_space=pl.ANY)
    return pl.pallas_call(
        functools.partial(gather_kernel, (n, CHUNKS, tile, quarter)),
        out_shape=(out, out),
        in_specs=[hbm] * 3,
        out_specs=(vmem, vmem),
        scratch_shapes=[
            pltpu.VMEM((n, piece, width), jnp.bfloat16),
            pltpu.VMEM((n * depth, 2 * cols), jnp.bfloat16),
        ]
        + [dma((steps,))] * 8
        + [dma((2 * n,))] * 6
        + [dma((3,))],
        compiler_params=pltpu.CompilerParams(
            collective_id=0, has_side_effects=True, vmem_limit_bytes=36 * 2**20
        ),
    )(prompt, w_key, w_value)


def read_kernel(
    pieces, query, key_new, value_new, lam, gain, k_all, v_all, keys, values, read,
    scores, out_sem,
):
    span, cols = k_all.shape
    tile = span // pieces
    heads = cols // VDIM
    me = lax.axis_index("sp")
    stores = (
        pltpu.make_async_copy(k_all, keys, out_sem.at[0]),
        pltpu.make_async_copy(v_all, values, out_sem.at[1]),
    )
    for copy in stores:
        copy.start()

    def mine(ref):
        whole = ref[...].astype(jnp.float32)
        here = lax.broadcasted_iota(jnp.int32, whole.shape, 0) == me
        return jnp.sum(jnp.where(here, whole, 0.0), axis=0, keepdims=True)

    shape = (2 * heads, cols)
    row = lax.broadcasted_iota(jnp.int32, shape, 0)
    group = lax.broadcasted_iota(jnp.int32, shape, 1) // HALF
    part = jnp.where(row < heads, 2 * row, 2 * (row - heads) + 1) == group
    q_row = mine(query)
    q_mat = jnp.where(part, jnp.broadcast_to(q_row, shape), 0.0)
    scale = HALF ** (-0.5)
    fresh = jnp.sum(q_mat * mine(key_new), axis=1, keepdims=True) * scale
    q_low = q_mat.astype(jnp.bfloat16)
    for i in range(pieces):
        scores[:, i * tile:(i + 1) * tile] = lax.dot_general(
            q_low, k_all[i * tile:(i + 1) * tile, :], (((1,), (1,)), ((), ())),
            preferred_element_type=jnp.float32,
        ) * scale
    s = scores[...]
    top = jnp.maximum(jnp.max(s, axis=1, keepdims=True), fresh)
    e = jnp.exp(s - top)
    own = jnp.exp(fresh - top)
    total = jnp.sum(e, axis=1, keepdims=True) + own
    w = e / total
    own = own / total
    mix = lam[...]
    mixed = (w[:heads] - mix * w[heads:]).astype(jnp.bfloat16)
    own_mixed = (own[:heads] - mix * own[heads:]).astype(jnp.bfloat16).astype(jnp.float32)
    o = jnp.dot(mixed, v_all[...], preferred_element_type=jnp.float32)
    o = o + own_mixed * mine(value_new)
    for h in range(heads):
        lanes = slice(h * VDIM, (h + 1) * VDIM)
        one = o[h:h + 1, lanes]
        mean = jnp.mean(one * one, axis=1, keepdims=True)
        read[:, lanes] = one * lax.rsqrt(mean + 1e-06) * gain[...]
    for copy in stores:
        copy.wait()


def read_call(query, key_new, value_new, mix_lambda, head_gain, keys, values):
    span, cols = keys.shape
    heads = mix_lambda.shape[0]
    pieces = 12
    hbm = pl.BlockSpec(memory_space=pl.ANY)
    vmem = pl.BlockSpec(memory_space=pltpu.VMEM)
    out = jax.ShapeDtypeStruct((span, cols), jnp.bfloat16)
    dma = pltpu.SemaphoreType.DMA
    return pl.pallas_call(
        functools.partial(read_kernel, pieces),
        out_shape=(out, out, jax.ShapeDtypeStruct((1, cols), jnp.float32)),
        in_specs=[vmem] * 7,
        out_specs=(hbm, hbm, vmem),
        scratch_shapes=[
            pltpu.VMEM((2 * heads, span), jnp.float32),
            dma((2,)),
        ],
        compiler_params=pltpu.CompilerParams(vmem_limit_bytes=32 * 2**20),
    )(query, key_new, value_new, mix_lambda[:, None], head_gain[None, :], keys, values)


def share_kernel(n, mine, out, slots, send_sem, recv_sem):
    me = lax.axis_index("sp")
    barrier = pltpu.get_barrier_semaphore()
    for step in range(1, n):
        pl.semaphore_signal(
            barrier, inc=1, device_id={"sp": lax.rem(me + step, n)}, device_id_type=MESH
        )
    pl.semaphore_wait(barrier, n - 1)

    def copy(step, src):
        return pltpu.make_async_remote_copy(
            src_ref=mine, dst_ref=slots.at[src],
            send_sem=send_sem.at[step], recv_sem=recv_sem.at[src],
            device_id={"sp": lax.rem(me + step, n)}, device_id_type=MESH,
        )

    for step in range(1, n):
        copy(step, me).start()
    for step in range(1, n):
        copy(step, lax.rem(me + step, n)).wait_recv()
    row = mine[...]
    for src in range(n):
        out[src:src + 1, :] = jnp.where(me == src, row, slots[src]).astype(jnp.bfloat16)
    for step in range(1, n):
        copy(step, me).wait_send()


def share(n, read):
    vmem = pl.BlockSpec(memory_space=pltpu.VMEM)
    dma = pltpu.SemaphoreType.DMA
    return pl.pallas_call(
        functools.partial(share_kernel, n),
        out_shape=jax.ShapeDtypeStruct((n, read.shape[1]), jnp.bfloat16),
        in_specs=[vmem],
        out_specs=vmem,
        scratch_shapes=[
            pltpu.VMEM((n, 1, read.shape[1]), jnp.float32), dma((n,)), dma((n,)),
        ],
        compiler_params=pltpu.CompilerParams(
            collective_id=1, has_side_effects=True, vmem_limit_bytes=2**20
        ),
    )(read)


def fast_body(prompt, w_key, w_value, query_new, key_new, value_new, mix_lambda, head_gain):
    count, piece, width = prompt.shape
    n = lax.axis_size("sp")
    keys, values = gather_project(n, prompt, w_key, w_value)
    cols = keys.shape[-1]
    keys, values, read = read_call(
        query_new, key_new, value_new, mix_lambda, head_gain,
        keys.reshape(n * piece, cols), values.reshape(n * piece, cols),
    )
    return (
        keys.reshape(1, n, piece, cols),
        values.reshape(1, n, piece, cols),
        share(n, read),
    )


def choose(mesh):
    def run(prompt, *rest):
        sizes = dict(mesh.shape)
        count, piece, width = prompt.shape
        rows = rest[0].shape[0]
        fits = (
            sizes["grp"] == 2
            and sizes["tp"] == 4
            and sizes["sp"] == count
            and count > 1
            and piece % (64 * CHUNKS) == 0
            and rows % 32 == 0
            and (count * piece) % 1536 == 0
            and count * piece * width * 2 <= 2**25
        )
        return (fast_body if fits else body)(prompt, *rest)

    return run


def solution(mesh):
    placed = (
        P("grp", "sp", None),
        P("sp", "tp"),
        P("sp", "tp"),
        P("grp", "tp"),
        P("grp", "tp"),
        P("grp", "tp"),
        P("tp"),
        P(),
    )
    return jax.shard_map(
        choose(mesh),
        mesh=mesh,
        in_specs=placed,
        out_specs=(
            P(("grp", "sp"), None, None, "tp"),
            P(("grp", "sp"), None, None, "tp"),
            P("grp", "tp"),
        ),
        check_vma=False,
    )
```

```python
import functools

import jax
import jax.numpy as jnp
from jax import lax
from jax.experimental import pallas as pl
from jax.experimental.pallas import tpu as pltpu
from jax.sharding import PartitionSpec as P

HALF = 64
VDIM = 128
MESH = pl.DeviceIdType.MESH
CHUNKS = 8
LAG_X = 1
LAG_C = 2
EARLY = 2
AHEAD = 24


def combined_all(part, axis, combine):
    gathered = jax.tree.map(lambda a: lax.all_gather(a, axis), part)

    def take(source):
        return jax.tree.map(lambda a: lax.dynamic_index_in_dim(a, source, 0, False), gathered)

    return lax.fori_loop(
        1, lax.axis_size(axis), lambda source, state: combine(state, take(source)), take(0)
    )


def project(rows, w_key, w_value):
    keys = jnp.dot(
        rows, lax.all_gather(w_key, "sp", axis=0, tiled=True), preferred_element_type=jnp.float32
    )
    values = jnp.dot(
        rows, lax.all_gather(w_value, "sp", axis=0, tiled=True), preferred_element_type=jnp.float32
    )
    return (keys.astype(jnp.bfloat16), values.astype(jnp.bfloat16))


def score_maps(query, keys):
    count, span = (keys.shape[0], keys.shape[1])
    heads = query.shape[1] // (2 * HALF)
    q_parts = query.reshape(count, heads, 2, HALF)
    k_parts = keys.reshape(count, span, heads, 2, HALF)
    return jnp.einsum(
        "shmc,slhmc->shml", q_parts, k_parts, preferred_element_type=jnp.float32
    ) * HALF ** (-0.5)


def own_scores(query, fresh_key):
    count = query.shape[0]
    heads = query.shape[1] // (2 * HALF)
    q_parts = query.astype(jnp.float32).reshape(count, heads, 2, HALF)
    k_parts = fresh_key.astype(jnp.float32).reshape(count, heads, 2, HALF)
    return jnp.sum(q_parts * k_parts, axis=-1) * HALF ** (-0.5)


def finish(reads, head_gain):
    mean = jnp.mean(reads * reads, axis=-1, keepdims=True)
    normed = reads * lax.rsqrt(mean + 1e-06) * head_gain
    return normed.reshape(reads.shape[0], -1).astype(jnp.bfloat16)


def join_totals(first, second):
    top = jnp.maximum(first[0], second[0])
    return (top, first[1] * jnp.exp(first[0] - top) + second[1] * jnp.exp(second[0] - top))


def placed(part_rows, prompts, first, fill):
    base = jnp.full((prompts,) + part_rows.shape[1:], fill, jnp.float32)
    return lax.dynamic_update_slice_in_dim(base, part_rows, first, 0)


def cache_read(query_new, key_new, value_new, keys, values, mix_lambda, head_gain, first):
    count, span = (keys.shape[0], keys.shape[1])
    prompts = query_new.shape[0]
    heads = mix_lambda.shape[0]
    query = lax.dynamic_slice_in_dim(query_new, first, count, 0)
    scores = score_maps(query, keys)
    fresh_all = own_scores(query_new, key_new)
    fresh = lax.dynamic_slice_in_dim(fresh_all, first, count, 0)
    local_top = jnp.maximum(jnp.max(scores, axis=-1), fresh)
    local_total = jnp.sum(jnp.exp(scores - local_top[..., None]), axis=-1)
    top_all, cache_total = combined_all(
        (placed(local_top, prompts, first, -1e30), placed(local_total, prompts, first, 0.0)),
        "sp",
        join_totals,
    )
    own = jnp.exp(fresh_all - top_all)
    total_all = cache_total + own
    top = lax.dynamic_slice_in_dim(top_all, first, count, 0)
    total = lax.dynamic_slice_in_dim(total_all, first, count, 0)
    probs = jnp.exp(scores - top[..., None]) / total[..., None]
    mixed = (probs[:, :, 0] - mix_lambda[None, :, None] * probs[:, :, 1]).astype(jnp.bfloat16)
    value_parts = values.reshape(count, span, heads, VDIM)
    partial_value = jnp.einsum(
        "shl,slhv->shv", mixed, value_parts, preferred_element_type=jnp.float32
    )
    reads = lax.psum(placed(partial_value, prompts, first, 0.0), "sp")
    own_prob = own / total_all
    own_mixed = (own_prob[:, :, 0] - mix_lambda[None, :] * own_prob[:, :, 1]).astype(jnp.bfloat16)
    reads = reads + own_mixed.astype(jnp.float32)[..., None] * value_new.astype(
        jnp.float32
    ).reshape(prompts, heads, VDIM)
    return finish(reads, head_gain)


def block_read(
    query_new, key_new, value_new, key_cache, value_cache, mix_lambda, head_gain, spread
):
    blocks, sub = (key_cache.shape[1], key_cache.shape[2])
    first = lax.axis_index("sp") // spread
    keys = key_cache.reshape(1, blocks * sub, -1)
    values = value_cache.reshape(1, blocks * sub, -1)
    return cache_read(query_new, key_new, value_new, keys, values, mix_lambda, head_gain, first)


def body(prompt, w_key, w_value, query_new, key_new, value_new, mix_lambda, head_gain):
    count, piece, width = prompt.shape
    spread = lax.axis_size("sp") // count
    sub = piece // spread
    keys, values = project(prompt.reshape(count * piece, width), w_key, w_value)
    key_blocks = keys.reshape(count * spread, 1, sub, -1)
    value_blocks = values.reshape(count * spread, 1, sub, -1)
    key_cache, value_cache = (
        lax.all_to_all(key_blocks, "sp", split_axis=0, concat_axis=1, tiled=True),
        lax.all_to_all(value_blocks, "sp", split_axis=0, concat_axis=1, tiled=True),
    )
    first_read = block_read(
        query_new, key_new, value_new, key_cache, value_cache, mix_lambda, head_gain, spread
    )
    return (key_cache, value_cache, first_read)


def gather_kernel(
    sizes, prompt, w_key, w_value, keys, values,
    rows_in, weights,
    z_send, z_recv, x_send, x_recv, d_send, d_recv, e_send, e_recv,
    wr_send, wr_recv, wl_send, wl_recv, wy_send, wy_recv, local,
):
    n, chunks, tile, quarter = sizes
    me = lax.axis_index("sp")
    tp = lax.axis_index("tp")
    grp = lax.axis_index("grp")
    across = lax.rem(tp + 2, 4)
    sibling = tp + 1 - 2 * lax.rem(tp, 2)
    far = lax.rem(sibling + 2, 4)
    depth, cols = w_key.shape
    half = depth // 2
    mats = (w_key, w_value)

    def rows(j, q):
        return pl.ds(pl.multiple_of(j * tile + q * quarter, quarter), quarter)

    barrier = pltpu.get_barrier_semaphore()
    for step in range(1, n):
        pl.semaphore_signal(
            barrier, inc=1, device_id={"sp": lax.rem(me + step, n)}, device_id_type=MESH
        )
    pl.semaphore_signal(barrier, inc=1, device_id={"tp": across}, device_id_type=MESH)
    pl.semaphore_signal(barrier, inc=1, device_id={"tp": sibling}, device_id_type=MESH)
    pl.semaphore_signal(barrier, inc=1, device_id={"grp": 1 - grp}, device_id_type=MESH)
    pl.semaphore_wait(barrier, n + 2)

    def w_slot(src, m, g):
        return weights.at[pl.ds(pl.multiple_of(src * depth + g * half, half), half),
                          pl.ds(m * cols, cols)]

    def w_hop(src, m, to, send, recv, own):
        origin = mats[m].at[pl.ds(pl.multiple_of(grp * half, half), half)] if own else w_slot(src, m, grp)
        return pltpu.make_async_remote_copy(
            src_ref=origin, dst_ref=w_slot(src, m, grp),
            send_sem=send.at[src * 2 + m], recv_sem=recv.at[src * 2 + m],
            device_id={"sp": to}, device_id_type=MESH,
        )

    def w_side(src, m, g):
        return pltpu.make_async_remote_copy(
            src_ref=w_slot(src, m, g), dst_ref=w_slot(src, m, g),
            send_sem=wy_send.at[src * 2 + m], recv_sem=wy_recv.at[src * 2 + m],
            device_id={"grp": 1 - grp}, device_id_type=MESH,
        )

    def z_copy(src, dst, j):
        return pltpu.make_async_remote_copy(
            src_ref=prompt.at[dst, rows(j, tp)], dst_ref=rows_in.at[src, rows(j, tp)],
            send_sem=z_send.at[dst * chunks + j], recv_sem=z_recv.at[src * chunks + j],
            device_id={"sp": dst}, device_id_type=MESH,
        )

    def side_copy(src, j, q, to, send, recv):
        return pltpu.make_async_remote_copy(
            src_ref=rows_in.at[src, rows(j, q)], dst_ref=rows_in.at[src, rows(j, q)],
            send_sem=send.at[src * chunks + j], recv_sem=recv.at[src * chunks + j],
            device_id={"tp": to}, device_id_type=MESH,
        )

    def right_send(i):
        @pl.when(i < (n - 1 - me) * chunks)
        def _():
            c = jnp.maximum(n - 1 - me, 1)
            z_copy(me, me + c - lax.rem(i, c), i // c).start()

    def left_send(i):
        @pl.when(i < me * chunks)
        def _():
            c = jnp.maximum(me, 1)
            z_copy(me, me - c + lax.rem(i, c), i // c).start()

    def both_sends(i, carry):
        right_send(i)
        left_send(i)
        return carry

    for m in range(2):
        @pl.when(me + 1 < n)
        def _():
            w_hop(me, m, me + 1, wr_send, wr_recv, True).start()

        @pl.when(me > 0)
        def _():
            w_hop(me, m, me - 1, wl_send, wl_recv, True).start()

    own_w = [
        pltpu.make_async_copy(
            mats[m],
            weights.at[pl.ds(pl.multiple_of(me * depth, depth), depth), pl.ds(m * cols, cols)],
            local.at[m],
        )
        for m in range(2)
    ]
    own_rows = pltpu.make_async_copy(prompt.at[me], rows_in.at[me], local.at[2])
    for copy in own_w:
        copy.start()
    own_rows.start()

    @pl.when(me == 0)
    def _():
        for i in range(EARLY):
            right_send(i)

    @pl.when(me == n - 1)
    def _():
        for i in range(EARLY):
            left_send(i)

    for d in range(1, n):
        @pl.when(me - d >= 0)
        def _():
            for m in range(2):
                w_hop(me - d, m, me, wr_send, wr_recv, False).wait_recv()

                @pl.when(me + 1 < n)
                def _():
                    w_hop(me - d, m, me + 1, wr_send, wr_recv, False).start()

                w_side(me - d, m, grp).start()

        @pl.when(me + d < n)
        def _():
            for m in range(2):
                w_hop(me + d, m, me, wl_send, wl_recv, False).wait_recv()

                @pl.when(me > 0)
                def _():
                    w_hop(me + d, m, me - 1, wl_send, wl_recv, False).start()

                w_side(me + d, m, grp).start()

        @pl.when(me == d)
        def _():
            for i in range(EARLY):
                right_send(i)

        @pl.when(n - 1 - me == d)
        def _():
            for i in range(EARLY):
                left_send(i)

    lax.fori_loop(EARLY, AHEAD, both_sends, 0)

    for step in range(1, n):
        src = lax.rem(me + step, n)
        for m in range(2):
            w_side(src, m, 1 - grp).wait_recv()
    for copy in own_w:
        copy.wait()
    own_rows.wait()

    def compute(src, j):
        where = pl.ds(pl.multiple_of(j * tile, tile), tile)
        both = jnp.dot(
            rows_in[src, where, :], weights[...], preferred_element_type=jnp.float32
        ).astype(jnp.bfloat16)
        keys[src, where, :] = both[:, :cols]
        values[src, where, :] = both[:, cols:]

    def order(k):
        pick = k * 0
        for spot in range(n):
            seq = []
            for j in range(chunks):
                for src in sorted(range(n), key=lambda a: -abs(a - spot)):
                    if src != spot:
                        slow = (src in (n // 2 - 1, n // 2)) and ((src < n // 2) != (spot < n // 2))
                        seq.append((j * 2 + (3 if slow else 0), len(seq), src * chunks + j))
            for at, (_, _, value) in enumerate(sorted(seq)):
                pick = jnp.where((me == spot) & (k == at), value, pick)
        return pick // chunks, lax.rem(pick, chunks)

    total = (n - 1) * chunks

    def step(k, carry):
        both_sends(AHEAD + k, 0)

        @pl.when(k < total)
        def _():
            src, j = order(k)
            z_copy(src, me, j).wait_recv()
            side_copy(src, j, tp, across, x_send, x_recv).start()
            side_copy(src, j, tp, sibling, d_send, d_recv).start()

        @pl.when((k >= LAG_X) & (k < total + LAG_X))
        def _():
            src, j = order(k - LAG_X)
            side_copy(src, j, across, across, x_send, x_recv).wait_recv()
            side_copy(src, j, across, sibling, e_send, e_recv).start()

        @pl.when(k < chunks)
        def _():
            compute(me, k)

        @pl.when(k >= LAG_C)
        def _():
            src, j = order(k - LAG_C)
            side_copy(src, j, sibling, sibling, d_send, d_recv).wait_recv()
            side_copy(src, j, far, sibling, e_send, e_recv).wait_recv()
            compute(src, j)

        return carry

    lax.fori_loop(0, total + LAG_C, step, 0)

    def drain(k, carry):
        src, j = order(k)
        z_copy(me, src, j).wait_send()
        side_copy(src, j, tp, across, x_send, x_recv).wait_send()
        side_copy(src, j, tp, sibling, d_send, d_recv).wait_send()
        side_copy(src, j, across, sibling, e_send, e_recv).wait_send()
        return carry

    lax.fori_loop(0, total, drain, 0)
    for step_ in range(1, n):
        src = lax.rem(me + step_, n)
        for m in range(2):
            w_side(src, m, grp).wait_send()
    for d in range(n):
        for m in range(2):
            @pl.when((me - d >= 0) & (me + 1 < n))
            def _():
                w_hop(me - d, m, me + 1, wr_send, wr_recv, False).wait_send()

            @pl.when((me + d < n) & (me > 0))
            def _():
                w_hop(me + d, m, me - 1, wl_send, wl_recv, False).wait_send()


def gather_project(n, prompt, w_key, w_value):
    count, piece, width = prompt.shape
    depth, cols = w_key.shape
    tile = piece // CHUNKS
    quarter = tile // 4
    dma = pltpu.SemaphoreType.DMA
    steps = n * CHUNKS
    out = pltpu.VMEM((n, piece, cols), jnp.bfloat16)
    vmem = pl.BlockSpec(memory_space=pltpu.VMEM)
    hbm = pl.BlockSpec(memory_space=pl.ANY)
    return pl.pallas_call(
        functools.partial(gather_kernel, (n, CHUNKS, tile, quarter)),
        out_shape=(out, out),
        in_specs=[hbm] * 3,
        out_specs=(vmem, vmem),
        scratch_shapes=[
            pltpu.VMEM((n, piece, width), jnp.bfloat16),
            pltpu.VMEM((n * depth, 2 * cols), jnp.bfloat16),
        ]
        + [dma((steps,))] * 8
        + [dma((2 * n,))] * 6
        + [dma((3,))],
        compiler_params=pltpu.CompilerParams(
            collective_id=0, has_side_effects=True, vmem_limit_bytes=36 * 2**20
        ),
    )(prompt, w_key, w_value)


def read_kernel(
    pieces, query, key_new, value_new, lam, gain, k_all, v_all, keys, values, read,
    scores, out_sem,
):
    span, cols = k_all.shape
    tile = span // pieces
    heads = cols // VDIM
    me = lax.axis_index("sp")
    stores = (
        pltpu.make_async_copy(k_all, keys, out_sem.at[0]),
        pltpu.make_async_copy(v_all, values, out_sem.at[1]),
    )
    for copy in stores:
        copy.start()

    def mine(ref):
        whole = ref[...].astype(jnp.float32)
        here = lax.broadcasted_iota(jnp.int32, whole.shape, 0) == me
        return jnp.sum(jnp.where(here, whole, 0.0), axis=0, keepdims=True)

    shape = (2 * heads, cols)
    row = lax.broadcasted_iota(jnp.int32, shape, 0)
    group = lax.broadcasted_iota(jnp.int32, shape, 1) // HALF
    part = jnp.where(row < heads, 2 * row, 2 * (row - heads) + 1) == group
    q_row = mine(query)
    q_mat = jnp.where(part, jnp.broadcast_to(q_row, shape), 0.0)
    scale = HALF ** (-0.5)
    fresh = jnp.sum(q_mat * mine(key_new), axis=1, keepdims=True) * scale
    q_low = q_mat.astype(jnp.bfloat16)
    for i in range(pieces):
        scores[:, i * tile:(i + 1) * tile] = lax.dot_general(
            q_low, k_all[i * tile:(i + 1) * tile, :], (((1,), (1,)), ((), ())),
            preferred_element_type=jnp.float32,
        ) * scale
    s = scores[...]
    top = jnp.maximum(jnp.max(s, axis=1, keepdims=True), fresh)
    e = jnp.exp(s - top)
    own = jnp.exp(fresh - top)
    total = jnp.sum(e, axis=1, keepdims=True) + own
    w = e / total
    own = own / total
    mix = lam[...]
    mixed = (w[:heads] - mix * w[heads:]).astype(jnp.bfloat16)
    own_mixed = (own[:heads] - mix * own[heads:]).astype(jnp.bfloat16).astype(jnp.float32)
    o = jnp.dot(mixed, v_all[...], preferred_element_type=jnp.float32)
    o = o + own_mixed * mine(value_new)
    for h in range(heads):
        lanes = slice(h * VDIM, (h + 1) * VDIM)
        one = o[h:h + 1, lanes]
        mean = jnp.mean(one * one, axis=1, keepdims=True)
        read[:, lanes] = one * lax.rsqrt(mean + 1e-06) * gain[...]
    for copy in stores:
        copy.wait()


def read_call(query, key_new, value_new, mix_lambda, head_gain, keys, values):
    span, cols = keys.shape
    heads = mix_lambda.shape[0]
    pieces = 12
    hbm = pl.BlockSpec(memory_space=pl.ANY)
    vmem = pl.BlockSpec(memory_space=pltpu.VMEM)
    out = jax.ShapeDtypeStruct((span, cols), jnp.bfloat16)
    dma = pltpu.SemaphoreType.DMA
    return pl.pallas_call(
        functools.partial(read_kernel, pieces),
        out_shape=(out, out, jax.ShapeDtypeStruct((1, cols), jnp.float32)),
        in_specs=[vmem] * 7,
        out_specs=(hbm, hbm, vmem),
        scratch_shapes=[
            pltpu.VMEM((2 * heads, span), jnp.float32),
            dma((2,)),
        ],
        compiler_params=pltpu.CompilerParams(vmem_limit_bytes=32 * 2**20),
    )(query, key_new, value_new, mix_lambda[:, None], head_gain[None, :], keys, values)


def share_kernel(n, mine, out, slots, send_sem, recv_sem):
    me = lax.axis_index("sp")
    barrier = pltpu.get_barrier_semaphore()
    for step in range(1, n):
        pl.semaphore_signal(
            barrier, inc=1, device_id={"sp": lax.rem(me + step, n)}, device_id_type=MESH
        )
    pl.semaphore_wait(barrier, n - 1)

    def copy(step, src):
        return pltpu.make_async_remote_copy(
            src_ref=mine, dst_ref=slots.at[src],
            send_sem=send_sem.at[step], recv_sem=recv_sem.at[src],
            device_id={"sp": lax.rem(me + step, n)}, device_id_type=MESH,
        )

    for step in range(1, n):
        copy(step, me).start()
    for step in range(1, n):
        copy(step, lax.rem(me + step, n)).wait_recv()
    row = mine[...]
    for src in range(n):
        out[src:src + 1, :] = jnp.where(me == src, row, slots[src]).astype(jnp.bfloat16)
    for step in range(1, n):
        copy(step, me).wait_send()


def share(n, read):
    vmem = pl.BlockSpec(memory_space=pltpu.VMEM)
    dma = pltpu.SemaphoreType.DMA
    return pl.pallas_call(
        functools.partial(share_kernel, n),
        out_shape=jax.ShapeDtypeStruct((n, read.shape[1]), jnp.bfloat16),
        in_specs=[vmem],
        out_specs=vmem,
        scratch_shapes=[
            pltpu.VMEM((n, 1, read.shape[1]), jnp.float32), dma((n,)), dma((n,)),
        ],
        compiler_params=pltpu.CompilerParams(
            collective_id=1, has_side_effects=True, vmem_limit_bytes=2**20
        ),
    )(read)


def fast_body(prompt, w_key, w_value, query_new, key_new, value_new, mix_lambda, head_gain):
    count, piece, width = prompt.shape
    n = lax.axis_size("sp")
    keys, values = gather_project(n, prompt, w_key, w_value)
    cols = keys.shape[-1]
    keys, values, read = read_call(
        query_new, key_new, value_new, mix_lambda, head_gain,
        keys.reshape(n * piece, cols), values.reshape(n * piece, cols),
    )
    return (
        keys.reshape(1, n, piece, cols),
        values.reshape(1, n, piece, cols),
        share(n, read),
    )


def choose(mesh):
    def run(prompt, *rest):
        sizes = dict(mesh.shape)
        count, piece, width = prompt.shape
        rows = rest[0].shape[0]
        fits = (
            sizes["grp"] == 2
            and sizes["tp"] == 4
            and sizes["sp"] == count
            and count > 1
            and piece % (64 * CHUNKS) == 0
            and rows % 32 == 0
            and (count * piece) % 1536 == 0
            and count * piece * width * 2 <= 2**25
        )
        return (fast_body if fits else body)(prompt, *rest)

    return run


def solution(mesh):
    placed = (
        P("grp", "sp", None),
        P("sp", "tp"),
        P("sp", "tp"),
        P("grp", "tp"),
        P("grp", "tp"),
        P("grp", "tp"),
        P("tp"),
        P(),
    )
    return jax.shard_map(
        choose(mesh),
        mesh=mesh,
        in_specs=placed,
        out_specs=(
            P(("grp", "sp"), None, None, "tp"),
            P(("grp", "sp"), None, None, "tp"),
            P("grp", "tp"),
        ),
        check_vma=False,
    )
```
